32 devices in a mesh: fs: 8 (over z, x), tp: 4 (over y, core).
Axes of the slice: x: 2, y: 2, z: 4, core: 2. Of those that a mesh axis runs over, the one named last changes fastest.
Arguments:
- tokens: bfloat16 [768, 4096], P('tp'), may hold values from -6 to 6
- norm_gain: float32 [4096], P('fs'), may hold values from 0.1 to 1.9
- gate_trained: float32 [4096, 11264], P('fs', 'tp'), may hold values from -0.09375 to 0.09375
- up_trained: float32 [4096, 11264], P('fs', 'tp'), may hold values from -0.09375 to 0.09375
- down_trained: float32 [11264, 4096], P('fs', 'tp'), may hold values from -0.078125 to 0.078125
Outputs:
- gate_sampler: bfloat16 [4096, 11264], P(None, 'fs')
- up_sampler: bfloat16 [4096, 11264], P(None, 'fs')
- down_sampler: bfloat16 [11264, 4096], P('fs')
- mixed_out: bfloat16 [768, 4096], P('tp', 'fs')
The draws below stay inside these ranges and needn't reach their ends.
All inputs are finite; a program needn't handle non-finite values.
Results may differ from the reference program's by a relative error of at most 0.0082.
Values may be sent and summed in bfloat16 or wider, within the bound.
No kernel may reach another device: no remote copies, remote signals or barrier semaphores. Data moves between devices by JAX's collectives and lax.ppermute only.
A program may use at most 128 MiB of HBM per device.

```python
import jax
import jax.numpy as jnp
from jax import lax

D = 4096
FF = 11264
TOKENS = 768


def spiked(entries, own_key, source, target, shards_of, factor):
    def block_of(axis_at):
        return (jnp.arange(entries.shape[axis_at]) // (entries.shape[axis_at] // shards_of)).reshape((-1,) + (1,) * (entries.ndim - 1 - axis_at))

    first = jax.random.permutation(own_key, shards_of)[block_of(target)]
    second = (block_of(target) + shards_of // 2) % shards_of
    return jnp.where((block_of(source) == first) | (block_of(source) == second), factor * entries, entries)


def shard_levels(rng, dims, shards, least, largest):
    loudness, own = 1.0, jax.random.fold_in(rng, 6)
    for dim, blocks in shards:
        steps = jnp.exp(jax.random.uniform(jax.random.fold_in(own, dim), (blocks,), jnp.float32, least / len(shards), largest / len(shards)))
        loudness = loudness * jnp.repeat(steps, dims[dim] // blocks).reshape([-1 if axis == dim else 1 for axis in range(len(dims))])
    return loudness


def gaussian(own_key, shape, scale, limit, cuts=(), kind=jnp.bfloat16):
    array = scale * jax.random.normal(own_key, shape, jnp.float32)
    if cuts:
        array = array * shard_levels(own_key, shape, cuts, -0.22, 0.18)
    return jnp.clip(array, -limit, limit).astype(kind)


def gaussian_with(rng, shape, scale, reach, split, heavy, held_as=jnp.bfloat16):
    values = scale * jax.random.normal(rng, shape, jnp.float32)
    if split:
        values = values * shard_levels(rng, shape, split, -0.22, 0.18)
    return jnp.clip(spiked(values, jax.random.fold_in(rng, 3), *heavy), -reach, reach).astype(held_as)


def setup_inputs(seed: int = 0) -> dict:
    key_list = jax.random.split(jax.random.key(seed), 6)
    tokens = gaussian(key_list[0], (TOKENS, D), 1.0, 6.0, ((0, 4),))
    norm_gain = jnp.clip(1.0 + 0.18 * jax.random.normal(key_list[1], (D,), jnp.float32), 0.1, 1.9)
    gate_trained = gaussian(key_list[2], (D, FF), D ** -0.5, 0.09375, ((0, 8), (1, 4)), jnp.float32)
    up_trained = gaussian(key_list[3], (D, FF), D ** -0.5, 0.09375, ((0, 8), (1, 4)), jnp.float32)
    down_trained = gaussian_with(key_list[4], (FF, D), FF ** -0.5, 0.078125, ((0, 8), (1, 4)), (0, 1, 8, 2.0), jnp.float32)
    return {"tokens": tokens, "norm_gain": norm_gain, "gate_trained": gate_trained, "up_trained": up_trained, "down_trained": down_trained}


def reference(tokens, norm_gain, gate_trained, up_trained, down_trained):
    gate_sampler = (norm_gain[:, None] * gate_trained).astype(jnp.bfloat16)
    up_sampler = (norm_gain[:, None] * up_trained).astype(jnp.bfloat16)
    down_sampler = down_trained.astype(jnp.bfloat16)
    as_float = tokens.astype(jnp.float32)
    normed = (as_float * jax.lax.rsqrt(lax.optimization_barrier(jnp.mean(as_float * as_float, axis=-1, keepdims=True)) + 1e-06)).astype(jnp.bfloat16)
    gate_act = jnp.dot(normed, gate_sampler, preferred_element_type=jnp.float32)
    up_act = jnp.dot(normed, up_sampler, preferred_element_type=jnp.float32)
    hidden = (jax.nn.silu(gate_act) * up_act).astype(jnp.bfloat16)
    mixed_out = jnp.dot(hidden, down_sampler, preferred_element_type=jnp.float32).astype(jnp.bfloat16)
    return (gate_sampler, up_sampler, down_sampler, mixed_out)
```

```python
import itertools

import jax
import jax.numpy as jnp
from jax import lax
from jax.experimental import pallas as pl
from jax.experimental.pallas import tpu as pltpu
from jax.sharding import PartitionSpec as P

BOTH = ("fs", "tp")
BF16 = jnp.bfloat16
F32 = jnp.float32


def normalise(tokens):
    as_float = tokens.astype(F32)
    return (
        as_float * lax.rsqrt(jnp.mean(as_float * as_float, axis=-1, keepdims=True) + 1e-06)
    ).astype(BF16)


def any_mesh(tokens, norm_gain, gate_trained, up_trained, down_trained):
    gate_local = (norm_gain[:, None] * gate_trained).astype(BF16)
    up_local = (norm_gain[:, None] * up_trained).astype(BF16)
    down_local = down_trained.astype(BF16)
    tp_count = lax.axis_size("tp")
    fs_count = lax.axis_size("fs")
    rows_local = gate_local.shape[0]
    cols_local = gate_local.shape[1]
    model_width = rows_local * fs_count
    owned_count = cols_local * tp_count // fs_count
    piece_cols = owned_count // tp_count
    block_count = cols_local // owned_count

    def arrange(matrix):
        return matrix.reshape(rows_local, block_count, tp_count, piece_cols)

    gate_mixed, up_mixed = (
        lax.all_to_all(arrange(gate_local), "tp", split_axis=2, concat_axis=2, tiled=True),
        lax.all_to_all(arrange(up_local), "tp", split_axis=2, concat_axis=2, tiled=True),
    )

    def regroup(matrix):
        return matrix.transpose(2, 1, 0, 3).reshape(fs_count, rows_local, piece_cols)

    gate_parts, up_parts = (
        lax.all_to_all(regroup(gate_mixed), "fs", split_axis=0, concat_axis=1, tiled=True),
        lax.all_to_all(regroup(up_mixed), "fs", split_axis=0, concat_axis=1, tiled=True),
    )
    gate_sampler, up_sampler, down_sampler = (
        lax.all_gather(gate_parts.reshape(model_width, piece_cols), "tp", axis=1, tiled=True),
        lax.all_gather(up_parts.reshape(model_width, piece_cols), "tp", axis=1, tiled=True),
        lax.all_gather(down_local, "tp", axis=1, tiled=True),
    )
    normed = normalise(tokens)
    gate_act = jnp.dot(normed, gate_sampler, preferred_element_type=F32)
    up_act = jnp.dot(normed, up_sampler, preferred_element_type=F32)
    hidden = (jax.nn.silu(gate_act) * up_act).astype(BF16)
    partial_terms = jnp.dot(hidden, down_sampler, preferred_element_type=F32)
    mixed_out = lax.psum_scatter(partial_terms, "fs", scatter_dimension=1, tiled=True).astype(BF16)
    return (gate_sampler, up_sampler, down_sampler, mixed_out)


def route(move, keep=lambda *place: True):
    def number(zh, zp, x, y, c):
        return ((zh * 2 + zp) * 2 + x) * 4 + y * 2 + c

    return [
        (number(*place), number(*move(*place)))
        for place in itertools.product(range(2), repeat=5)
        if keep(*place)
    ]


CROSS = route(lambda zh, zp, x, y, c: (zh, zp, x, 1 - y, c))
HOME_CROSS = route(lambda zh, zp, x, y, c: (zh, zp, x, 1 - y, c), lambda zh, zp, x, y, c: zh == y)
CORE = route(lambda zh, zp, x, y, c: (zh, zp, x, y, 1 - c))
NEAR = [route(lambda zh, zp, x, y, c, d=d: (zh, c, x ^ d, y, zp)) for d in range(2)]
FAR = [route(lambda zh, zp, x, y, c, d=d: (1 - zh, c, x ^ d, y, zp)) for d in range(2)]
FLIP_X = route(lambda zh, zp, x, y, c: (zh, zp, 1 - x, y, c))
FLIP_ZP = route(lambda zh, zp, x, y, c: (zh, 1 - zp, x, y, c))
TO_HOME = route(lambda zh, zp, x, y, c: (1 - zh, zp, x, y, c), lambda zh, zp, x, y, c: zh != y)
TO_AWAY = route(lambda zh, zp, x, y, c: (1 - zh, zp, x, y, c), lambda zh, zp, x, y, c: zh == y)


def send(value, pairs):
    return lax.ppermute(value, BOTH, pairs)


def fold_kernel(pick_ref, gain_top, gain_low, top, low, a_ref, b_ref, p_ref):
    a = (gain_top[...] * top[...]).astype(BF16)
    b = (gain_low[...] * low[...]).astype(BF16)
    a_ref[...] = a
    b_ref[...] = b
    p_ref[...] = jnp.where(pick_ref[1] > 0, a, b)


def fold_gain(gain, matrix, half_col, is_home):
    rows, cols = matrix.shape
    half, width = rows // 2, cols // 2
    steps = 2
    tile = half // steps
    pick = jnp.stack([half_col, is_home.astype(jnp.int32)])
    out = jax.ShapeDtypeStruct((half, width), BF16)
    return pl.pallas_call(
        fold_kernel,
        grid_spec=pltpu.PrefetchScalarGridSpec(
            num_scalar_prefetch=1,
            grid=(steps,),
            in_specs=[
                pl.BlockSpec((tile, 1), lambda i, s: (i, 0)),
                pl.BlockSpec((tile, 1), lambda i, s: (i + steps, 0)),
                pl.BlockSpec((tile, width), lambda i, s: (i, s[0])),
                pl.BlockSpec((tile, width), lambda i, s: (i + steps, s[0])),
            ],
            out_specs=[pl.BlockSpec((tile, width), lambda i, s: (i, 0))] * 3,
        ),
        out_shape=[out] * 3,
        cost_estimate=pl.CostEstimate(
            flops=rows * width * 400, bytes_accessed=rows * width * 7, transcendentals=0
        ),
        name="fold_gain",
    )(pick, gain, gain, matrix, matrix)


def absorb_kernel(count, first, *refs):
    index = refs[0]
    normed = refs[1 : 1 + count]
    pieces = refs[1 + count : 1 + 2 * count]
    act_in, act, whole, sems = refs[1 + 2 * count], refs[-3], refs[-2], refs[-1]
    copies = [
        pltpu.make_async_copy(pieces[k], whole.at[index[k]], sems.at[k]) for k in range(count)
    ]
    for copy in copies:
        copy.start()
    if first:
        total = jnp.zeros(act.shape, F32)
    else:
        total = act_in[...]
    for k in range(count):
        total += jnp.dot(normed[k][0], pieces[k][...], preferred_element_type=F32)
    act[...] = total
    for copy in copies:
        copy.wait()


def absorb(normed, pieces, places, act, whole):
    count = len(pieces)
    blocks, tokens, depth = normed.shape
    width = pieces[0].shape[1]
    first = act is None
    vmem = pl.BlockSpec(memory_space=pltpu.VMEM)
    hbm = pl.BlockSpec(memory_space=pl.ANY)
    operands = [jnp.stack(places)] + [normed] * count + list(pieces)
    specs = [
        pl.BlockSpec((1, tokens, depth), lambda i, s, k=k: (s[k], 0, 0)) for k in range(count)
    ]
    specs += [pl.BlockSpec((depth, width), lambda i, s: (0, 0))] * count
    aliases = {}
    act_spec = pl.BlockSpec((tokens, width), lambda i, s: (0, 0))
    if first:
        operands.append(places[0].reshape(1))
        specs.append(pl.BlockSpec(memory_space=pltpu.SMEM))
    else:
        aliases = {len(operands): 0, len(operands) + 1: 1}
        operands += [act, whole]
        specs += [act_spec, hbm]
    return pl.pallas_call(
        lambda *refs: absorb_kernel(count, first, *refs),
        grid_spec=pltpu.PrefetchScalarGridSpec(
            num_scalar_prefetch=1,
            grid=(1,),
            in_specs=specs,
            out_specs=[act_spec, hbm],
            scratch_shapes=[pltpu.SemaphoreType.DMA((count,))],
        ),
        out_shape=[
            jax.ShapeDtypeStruct((tokens, width), F32),
            jax.ShapeDtypeStruct((blocks, depth, width), BF16),
        ],
        input_output_aliases=aliases,
        compiler_params=pltpu.CompilerParams(vmem_limit_bytes=32 * 2**20),
        cost_estimate=pl.CostEstimate(
            flops=2 * count * tokens * depth * width,
            bytes_accessed=4 * count * depth * width + 8 * tokens * width,
            transcendentals=0,
        ),
        name="absorb",
    )(*operands)


def place_kernel(index, piece, *refs):
    refs[-1][...] = piece[...]


def place_columns(piece, column, whole, count):
    rows, width = piece.shape
    steps = 4
    tile = rows // steps
    operands = [column.reshape(1), piece]
    specs = [pl.BlockSpec((tile, width), lambda i, s: (i, 0))]
    aliases = {}
    if whole is not None:
        operands.append(whole)
        specs.append(pl.BlockSpec(memory_space=pl.ANY))
        aliases = {2: 0}
    return pl.pallas_call(
        place_kernel,
        grid_spec=pltpu.PrefetchScalarGridSpec(
            num_scalar_prefetch=1,
            grid=(steps,),
            in_specs=specs,
            out_specs=pl.BlockSpec((tile, width), lambda i, s: (i, s[0])),
        ),
        out_shape=jax.ShapeDtypeStruct((rows, width * count), BF16),
        input_output_aliases=aliases,
        cost_estimate=pl.CostEstimate(
            flops=rows * width * 400, bytes_accessed=rows * width * 4, transcendentals=0
        ),
        name="place",
    )(*operands)


def after(value, *others):
    return lax.optimization_barrier((value,) + others)[0]


def routed(tokens, norm_gain, gate_trained, up_trained, down_trained):
    fs, tp = lax.axis_index("fs"), lax.axis_index("tp")
    zh, zp, x = fs // 4, fs // 2 % 2, fs % 2
    y, c = tp // 2, tp % 2
    is_home = zh == y
    rows = gate_trained.shape[0]
    half = rows // 2
    width = gate_trained.shape[1] // 2
    blocks = 2 * lax.axis_size("fs")
    gain = norm_gain[:, None]
    far_half = jnp.where(is_home, 0, 1)

    def block(z_half, core, d, part):
        return (((z_half * 2 + core) * 2 + (x ^ d)) * 2 + part).astype(jnp.int32)

    token_rows = tokens.shape[0]
    normed = normalise(tokens).reshape(token_rows, blocks, half).transpose(1, 0, 2)

    lanes = []
    for matrix in (gate_trained, up_trained):
        for d in range(2):
            a, b, p = fold_gain(gain, matrix, x ^ d, is_home)
            lanes.append(dict(a=a, b=b, p=p, d=d))
    down_local = down_trained.astype(BF16)
    down_pair = send(down_local, CORE)
    for lane in lanes:
        lane["ra"] = send(lane["p"], CROSS)
    for lane in lanes:
        d, a, ra = lane["d"], lane["a"], lane["ra"]
        lane["far"] = send(jnp.where(is_home, ra, a), FAR[d])
        lane["near0"] = send(jnp.where(is_home, a, ra), NEAR[d])
    for lane in lanes:
        lane["rb"] = send(lane["b"], HOME_CROSS)
    for lane in lanes:
        d = lane["d"]
        lane["near1"] = send(jnp.where(is_home, lane["b"], lane["rb"]), NEAR[d])
    for lane in lanes:
        lane["far_other"] = send(lane["far"], CROSS)

    acts, wholes = [None, None], [None, None]

    def take(number, lane, names, spots):
        m = number // 2
        pieces, places = [], []
        for name, (z_half, part) in zip(names, spots):
            piece = lane[name]
            pieces += [piece, send(piece, CORE)]
            places += [block(z_half, c, lane["d"], part), block(z_half, 1 - c, lane["d"], part)]
        acts[m], wholes[m] = absorb(normed, pieces, places, acts[m], wholes[m])

    for number, lane in enumerate(lanes):
        take(number, lane, ("near0", "near1"), ((zh, 0), (zh, 1)))
    for number, lane in enumerate(lanes):
        take(number, lane, ("far",), ((1 - zh, far_half),))
        take(number, lane, ("far_other",), ((1 - zh, 1 - far_half),))

    gate_act, up_act = acts
    hidden = (jax.nn.silu(gate_act) * up_act).astype(BF16)

    down_cross = send(after(down_local, lanes[-1]["far"]), CROSS)
    down_cross_pair = send(down_cross, CORE)
    count = lax.axis_size("tp")
    down_whole = None
    for piece, column in (
        (down_local, tp),
        (down_pair, tp ^ 1),
        (down_cross, tp ^ 2),
        (down_cross_pair, tp ^ 3),
    ):
        down_whole = place_columns(piece, column.astype(jnp.int32), down_whole, count)

    owner_cols = down_local.shape[1] // 2

    def reduce_to(own, pair, last):
        mine = jnp.dot(hidden, own, preferred_element_type=F32)
        other = jnp.dot(hidden, pair, preferred_element_type=F32)
        low = jnp.where(c == 0, mine, other).reshape(token_rows, 2, owner_cols)
        high = jnp.where(c == 0, other, mine).reshape(token_rows, 2, owner_cols)
        got = []
        for part in (low, high):
            away = jnp.where(x == 0, part[:, 1], part[:, 0]).astype(BF16)
            keep = jnp.where(x == 0, part[:, 0], part[:, 1])
            got.append(keep + send(away, FLIP_X).astype(F32))
        away = jnp.where(zp == 0, got[1], got[0]).astype(BF16)
        keep = jnp.where(zp == 0, got[0], got[1])
        total = keep + send(away, FLIP_ZP).astype(F32)
        return total + send(total.astype(BF16), last).astype(F32)

    to_home = reduce_to(down_local, down_pair, TO_HOME)
    to_away = reduce_to(down_cross, down_cross_pair, TO_AWAY)
    mixed_out = jnp.where(is_home, to_home, to_away).astype(BF16)
    model_width = rows * lax.axis_size("fs")
    return (
        wholes[0].reshape(model_width, width),
        wholes[1].reshape(model_width, width),
        down_whole,
        mixed_out,
    )


def solution(mesh):
    in_specs = (P("tp", None), P("fs"), P("fs", "tp"), P("fs", "tp"), P("fs", "tp"))
    out_specs = (P(None, "fs"), P(None, "fs"), P("fs", None), P("tp", "fs"))
    cube = mesh.shape["fs"] == 2**3 and mesh.shape["tp"] == 2**2
    return jax.shard_map(
        routed if cube else any_mesh,
        mesh=mesh,
        in_specs=in_specs,
        out_specs=out_specs,
        check_vma=False,
    )
```
